1024 devices in a mesh: grp: 2 (over x), sp: 16 (over z), tp: 32 (over y, core).
Axes of the slice: x: 2, y: 16, z: 16, core: 2. Of those that a mesh axis runs over, the one named last changes fastest.
The devices are a block of a 4x16x16 slice.
Arguments:
- grid_tokens: bfloat16 [256, 512, 1024], P(('grp', 'sp'), 'tp'), parts along dimension 0, may hold values from -6 to 6
- norm_gain: float32 [2, 1024], replicated, may hold values from 0.1 to 1.9
- w_query: bfloat16 [2, 1024, 512], replicated, may hold values from -0.84375 to 0.84375
- w_key: bfloat16 [2, 1024, 512], replicated, may hold values from -1.1390625 to 1.1390625
- w_value: bfloat16 [2, 1024, 512], replicated, may hold values from -0.1875 to 0.1875
- offset_bias: float32 [2, 4, 15, 31], replicated, may hold values from -5 to 5
- w_out: bfloat16 [2, 512, 1024], replicated, may hold values from -1 to 1
Outputs:
- grid_out: bfloat16 [256, 512, 1024], P(('grp', 'sp'), 'tp'), parts along dimension 0
The draws below stay inside these ranges and needn't reach their ends.
There are 2 independent parts, one for each index of `grp`. The reference program is written for one: setup_inputs(seed, part) draws one part's arguments, and reference() takes and returns one part's arrays. A program takes and returns all parts, laid end to end along the dimension named above; an argument that names none is the same for every part. Nothing has to cross between parts.
All inputs are finite; a program needn't handle non-finite values.
Results may differ from the reference program's by a relative error of at most 0.014.
Values may be sent and summed in bfloat16 or wider, within the bound.
No kernel may reach another device: no remote copies, remote signals or barrier semaphores. Data moves between devices by JAX's collectives and lax.ppermute only.
A program may use at most 64 MiB of HBM per device.

```python
import jax
import jax.numpy as jnp
from jax import lax

D = 1024
HEADS = 4
HEAD_DIM = 128
WIN_ROWS = 8
WIN_COLS = 16
LAYERS = 2
GRID_ROWS = 128
GRID_COLS = 512


def query_key_pair(key):
    base = jax.random.fold_in(key, 7)
    first_key, second_key = jax.random.split(base, 2)
    shape = (LAYERS, D, HEADS * HEAD_DIM)
    first = jnp.clip(jax.random.normal(first_key, shape, jnp.float32), -6.0, 6.0)
    second = jnp.clip(jax.random.normal(second_key, shape, jnp.float32), -6.0, 6.0)
    query_part = first
    key_part = second
    factor = D ** (-0.5)
    return (query_part * factor, key_part * factor)


def draw_w_query(key, part):
    return query_key_pair(key)[0].astype(jnp.bfloat16)


def draw_w_key(key, part):
    return query_key_pair(key)[1].astype(jnp.bfloat16)


def shard_levels(key, shape, cuts, smallest, high):
    def one(dim, parts):
        steps = jax.random.uniform(jax.random.fold_in(jax.random.fold_in(key, 6), dim), (parts,), jnp.float32, smallest / len(cuts), high / len(cuts))
        return jnp.repeat(jnp.exp(steps), shape[dim] // parts).reshape((-1,) + (1,) * (len(shape) - dim - 1))

    factor_of = one(*cuts[0])
    for cut in cuts[1:]:
        factor_of = factor_of * one(*cut)
    return factor_of


def scatter_about(key, extent, spread, reach, cuts=(), kind=jnp.bfloat16):
    drawn = spread * jax.random.normal(key, extent, jnp.float32)
    if cuts:
        drawn = drawn * shard_levels(key, extent, cuts, -0.22, 0.18)
    return jnp.clip(drawn, -reach, reach).astype(kind)


def setup_inputs(seed: int = 0, part: int = 0) -> dict:
    key_of = jax.random.split(jax.random.key(seed), 8)
    own_keys = jax.random.split(jax.random.fold_in(key_of[7], part), 8)
    grid_tokens = scatter_about(own_keys[0], (GRID_ROWS, GRID_COLS, D), 1.0, 6.0, ((0, 16), (1, 32)))
    norm_gain = jnp.clip(1.0 + 0.18 * jax.random.normal(key_of[1], (LAYERS, D), jnp.float32), 0.1, 1.9)
    w_query = draw_w_query(jax.random.fold_in(key_of[7], 71), part)
    w_key = draw_w_key(jax.random.fold_in(key_of[7], 71), part)
    w_value = scatter_about(key_of[4], (LAYERS, D, HEADS * HEAD_DIM), D ** -0.5, 0.1875)
    offset_bias = scatter_about(key_of[5], (LAYERS, HEADS, 2 * WIN_ROWS - 1, 2 * WIN_COLS - 1), 1.0, 5.0, (), jnp.float32)
    w_out = scatter_about(key_of[6], (LAYERS, HEADS * HEAD_DIM, D), (HEADS * HEAD_DIM // 16) ** -0.5, 1.0)
    return dict(grid_tokens=grid_tokens, norm_gain=norm_gain, w_query=w_query, w_key=w_key, w_value=w_value, offset_bias=offset_bias, w_out=w_out)


NORM_EPSILON = 1e-06

def rms_rows(stream, gain):
    values = stream.astype(jnp.float32)
    factor = lax.rsqrt(lax.optimization_barrier(jnp.mean(values * values, axis=-1, keepdims=True)) + NORM_EPSILON)
    return (values * factor * gain).astype(jnp.bfloat16)

def window_mix(queries, keys_in, values_in, bias_table):
    grid_rows, grid_cols, inner = queries.shape
    head_count = bias_table.shape[0]
    inv_root = 1.0 / HEAD_DIM ** 0.5
    col_ids = jnp.arange(grid_cols, dtype=jnp.int32)
    col_start = jnp.clip(col_ids - WIN_COLS // 2, 0, grid_cols - WIN_COLS)
    key_cols = col_start[:, None] + jnp.arange(WIN_COLS, dtype=jnp.int32)[None, :]
    col_offsets = key_cols - col_ids[:, None] + WIN_COLS - 1
    col_bias = bias_table[:, :, col_offsets]

    def one_row(row_id):
        row_start = jnp.clip(row_id - WIN_ROWS // 2, 0, grid_rows - WIN_ROWS).astype(jnp.int32)
        key_rows = lax.dynamic_slice_in_dim(keys_in, row_start, WIN_ROWS, 0)
        value_rows = lax.dynamic_slice_in_dim(values_in, row_start, WIN_ROWS, 0)
        near_keys = key_rows[:, key_cols].reshape(WIN_ROWS, grid_cols, WIN_COLS, head_count, HEAD_DIM).astype(jnp.float32)
        near_values = value_rows[:, key_cols].reshape(WIN_ROWS, grid_cols, WIN_COLS, head_count, HEAD_DIM).astype(jnp.float32)
        row_query = lax.dynamic_index_in_dim(queries, row_id, 0, keepdims=False)
        row_query = row_query.reshape(grid_cols, head_count, HEAD_DIM).astype(jnp.float32)
        scores = jnp.einsum('chd,jckhd->hcjk', row_query, near_keys) * inv_root
        row_offsets = row_start + jnp.arange(WIN_ROWS, dtype=jnp.int32) - row_id + WIN_ROWS - 1
        offset_terms = jnp.take(col_bias, row_offsets, axis=1)
        scores = scores + jnp.transpose(offset_terms, (0, 2, 1, 3))
        top = lax.optimization_barrier(jnp.max(scores, axis=(2, 3), keepdims=True))
        expo = jnp.exp(scores - top)
        attn_weights = (expo / lax.optimization_barrier(jnp.sum(expo, axis=(2, 3), keepdims=True))).astype(jnp.bfloat16)
        mixture = jnp.einsum('hcjk,jckhd->chd', attn_weights.astype(jnp.float32), near_values)
        return mixture.astype(jnp.bfloat16).reshape(grid_cols, inner)
    return lax.map(one_row, jnp.arange(grid_rows, dtype=jnp.int32))

def reference(grid_tokens, norm_gain, w_query, w_key, w_value, offset_bias, w_out):
    stream = grid_tokens
    for layer_index in range(LAYERS):
        normed = rms_rows(stream, norm_gain[layer_index])
        queries = jnp.dot(normed, w_query[layer_index], preferred_element_type=jnp.float32).astype(jnp.bfloat16)
        keys_all = jnp.dot(normed, w_key[layer_index], preferred_element_type=jnp.float32).astype(jnp.bfloat16)
        values_all = jnp.dot(normed, w_value[layer_index], preferred_element_type=jnp.float32).astype(jnp.bfloat16)
        mixture = window_mix(queries, keys_all, values_all, offset_bias[layer_index])
        branch = jnp.dot(mixture, w_out[layer_index], preferred_element_type=jnp.float32)
        stream = (stream.astype(jnp.float32) + branch).astype(jnp.bfloat16)
    return stream
```

```python
import functools
import math

import jax
import jax.numpy as jnp
from jax import lax
from jax.experimental import pallas as pl
from jax.experimental.pallas import tpu as pltpu
from jax.sharding import PartitionSpec as P

HEAD_DIM = 128
WIN_ROWS = 8
WIN_COLS = 16
LAYERS = 2
HALF_ROWS = WIN_ROWS // 2
HALF_COLS = WIN_COLS // 2

NORM_EPSILON = 1e-06
LOG2E = math.log2(math.e)
MASKED = -1e30

BLOCK_ROWS = 8
BLOCK_COLS = 16
SLAB_ROWS = BLOCK_ROWS + WIN_ROWS
SLAB_COLS = BLOCK_COLS + WIN_COLS
QUERIES = BLOCK_ROWS * BLOCK_COLS
SLAB = SLAB_ROWS * SLAB_COLS
LANES = 128
GROUP = LANES // SLAB_COLS
SPAN = SLAB_ROWS - GROUP + BLOCK_ROWS
BLOCKS = 5

VMEM = pl.BlockSpec(memory_space=pltpu.VMEM)


def bias_rows(table):
    before = HALF_ROWS
    after = SPAN + GROUP - 1 - before - table.shape[2]
    rows = jnp.pad(
        table * LOG2E, ((0, 0), (0, 0), (before, after), (0, SLAB_COLS - table.shape[3]))
    )
    return jnp.concatenate([rows[:, :, g : g + SPAN] for g in range(GROUP)], axis=3)


def bias_kernel(grid_rows, grid_cols, tile_rows, tile_cols, rows_ref, out_ref, shifted):
    layers, heads = rows_ref.shape[:2]
    first_row = lax.axis_index("sp") * tile_rows
    first_col = lax.axis_index("tp") * tile_cols

    def shift(index, _):
        layer, head = index // heads, index % heads
        for u in range(SPAN):
            line = jnp.broadcast_to(rows_ref[layer, head, u : u + 1], (BLOCK_COLS, LANES))
            shifted[layer, head, u] = pltpu.roll(
                line, LANES - (HALF_COLS - 1), 1, stride=1, stride_axis=0
            )
        return 0

    lax.fori_loop(0, layers * heads, shift, 0)
    lane = lax.broadcasted_iota(jnp.int32, (BLOCK_COLS, LANES), 1)
    column = lax.broadcasted_iota(jnp.int32, (BLOCK_COLS, LANES), 0)
    key_col = lane % SLAB_COLS
    key_row = lane // SLAB_COLS

    def block(index, _):
        last = index // (BLOCKS - 1)
        row_block, col_block = (index // 2) % 2, index % 2
        row0 = first_row + (1 - last) * (row_block * BLOCK_ROWS - HALF_ROWS)
        col0 = first_col + (1 - last) * (col_block * BLOCK_COLS - HALF_COLS)
        col_start = jnp.clip(col0 + column - HALF_COLS, 0, grid_cols - WIN_COLS)
        behind = col0 - HALF_COLS + key_col - col_start
        col_inside = (behind >= 0) & (behind < WIN_COLS)
        for i in range(BLOCK_ROWS):
            row_start = jnp.clip(row0 + i - HALF_ROWS, 0, grid_rows - WIN_ROWS)
            for j in range(SLAB_ROWS // GROUP):
                below = key_row + (row0 - HALF_ROWS + j * GROUP - row_start)
                inside = col_inside & (below >= 0) & (below < WIN_ROWS)
                for head in range(heads):
                    out_ref[
                        index,
                        head,
                        i * BLOCK_COLS : (i + 1) * BLOCK_COLS,
                        j * LANES : (j + 1) * LANES,
                    ] = jnp.where(
                        inside, shifted[last, head, GROUP * j - i + BLOCK_ROWS - 1], MASKED
                    )
        return 0

    lax.fori_loop(0, BLOCKS, block, 0)


def normed_rows(values, gain):
    factor = lax.rsqrt(jnp.mean(values * values, axis=-1, keepdims=True) + NORM_EPSILON)
    return values * factor * gain


def project(cells, weight):
    rows, cols, width = cells.shape
    out = jnp.dot(
        cells.reshape(rows * cols, width), weight, preferred_element_type=jnp.float32
    )
    return out.astype(jnp.bfloat16).reshape(rows, cols, weight.shape[1])


def attend(queries, keys, values, bias):
    scores = lax.dot_general(
        queries.reshape(QUERIES, HEAD_DIM),
        keys.reshape(SLAB, HEAD_DIM),
        (((1,), (1,)), ((), ())),
        preferred_element_type=jnp.float32,
    )
    scores = scores * (LOG2E / HEAD_DIM**0.5) + bias
    expo = jnp.exp2(scores - jnp.max(scores, axis=1, keepdims=True))
    total = jnp.sum(expo, axis=1, keepdims=True)
    mixture = jnp.dot(
        expo.astype(jnp.bfloat16),
        values.reshape(SLAB, HEAD_DIM),
        preferred_element_type=jnp.float32,
    )
    return (mixture / total).astype(jnp.bfloat16).reshape(BLOCK_ROWS, BLOCK_COLS, HEAD_DIM)


def layers_kernel(
    left,
    mid,
    right,
    gain,
    w_query,
    w_key,
    w_value,
    w_out,
    bias,
    out_ref,
    normed,
    normed_q,
    keys,
    values,
    queries,
    mixture,
    branch,
    center,
):
    f32, bf16 = jnp.float32, jnp.bfloat16
    heads = w_query.shape[2] // HEAD_DIM
    region_rows, region_cols = mixture.shape[:2]

    def norm_first(r, _):
        parts = [normed_rows(ref[r].astype(f32), gain[0:1]) for ref in (left, mid, right)]
        for index, part in enumerate(parts):
            normed[r, index * BLOCK_COLS : (index + 1) * BLOCK_COLS] = part.astype(bf16)
        for index in range(2):
            both = (parts[index][HALF_COLS:], parts[index + 1][:HALF_COLS])
            normed_q[r, index * BLOCK_COLS : (index + 1) * BLOCK_COLS] = jnp.concatenate(
                both, axis=0
            ).astype(bf16)
        return 0

    lax.fori_loop(0, left.shape[0], norm_first, 0)
    keys[...] = project(normed[...], w_key[0])
    values[...] = project(normed[...], w_value[0])
    queries[...] = project(normed_q[HALF_ROWS : HALF_ROWS + region_rows], w_query[0])

    def first_block(index, _):
        row = index // 2 * BLOCK_ROWS
        col = pl.multiple_of(index % 2 * BLOCK_COLS, BLOCK_COLS)
        tile = (pl.ds(row, BLOCK_ROWS), pl.ds(col, BLOCK_COLS))
        slab = (pl.ds(row, SLAB_ROWS), pl.ds(col, SLAB_COLS))
        for head in range(heads):
            lanes = pl.ds(head * HEAD_DIM, HEAD_DIM)
            mixture[(*tile, lanes)] = attend(
                queries[(*tile, lanes)],
                keys[(*slab, lanes)],
                values[(*slab, lanes)],
                bias[index, head],
            )
        return 0

    lax.fori_loop(0, BLOCKS - 1, first_block, 0)
    branch[...] = jnp.dot(
        mixture[...].reshape(region_rows * region_cols, heads * HEAD_DIM),
        w_out[0],
        preferred_element_type=f32,
    ).reshape(branch.shape)

    def norm_second(r, _):
        tokens = jnp.concatenate(
            (
                left[r + HALF_ROWS].astype(f32)[HALF_COLS:],
                mid[r + HALF_ROWS].astype(f32),
                right[r + HALF_ROWS].astype(f32)[:HALF_COLS],
            ),
            axis=0,
        )
        stream = (tokens + branch[r]).astype(bf16).astype(f32)
        part = normed_rows(stream, gain[1:2])
        normed[r, :region_cols] = part.astype(bf16)
        normed_q[r, :BLOCK_COLS] = part[HALF_COLS : HALF_COLS + BLOCK_COLS].astype(bf16)
        center[r] = stream[HALF_COLS : HALF_COLS + BLOCK_COLS]
        return 0

    lax.fori_loop(0, region_rows, norm_second, 0)
    own = pl.ds(HALF_ROWS, BLOCK_ROWS)
    keys[:region_rows, :region_cols] = project(normed[:region_rows, :region_cols], w_key[1])
    values[:region_rows, :region_cols] = project(normed[:region_rows, :region_cols], w_value[1])
    queries[:BLOCK_ROWS, :BLOCK_COLS] = project(normed_q[own, :BLOCK_COLS], w_query[1])
    for head in range(heads):
        lanes = pl.ds(head * HEAD_DIM, HEAD_DIM)
        mixture[:BLOCK_ROWS, :BLOCK_COLS, lanes] = attend(
            queries[:BLOCK_ROWS, :BLOCK_COLS, lanes],
            keys[:SLAB_ROWS, :SLAB_COLS, lanes],
            values[:SLAB_ROWS, :SLAB_COLS, lanes],
            bias[BLOCKS - 1, head],
        )
    last = jnp.dot(
        mixture[:BLOCK_ROWS, :BLOCK_COLS].reshape(QUERIES, heads * HEAD_DIM),
        w_out[1],
        preferred_element_type=f32,
    )
    out_ref[...] = (center[own] + last.reshape(out_ref.shape)).astype(out_ref.dtype)


def shifts(cells, axis):
    ends = lax.axis_size(axis) - 1
    before = lax.ppermute(cells, axis, [(i, i + 1) for i in range(ends)])
    after = lax.ppermute(cells, axis, [(i + 1, i) for i in range(ends)])
    return before, after


def on_device(grid_tokens, norm_gain, w_query, w_key, w_value, offset_bias, w_out):
    tile_rows, tile_cols, width = grid_tokens.shape
    grid_rows = tile_rows * lax.axis_size("sp")
    grid_cols = tile_cols * lax.axis_size("tp")
    heads = offset_bias.shape[1]
    inner = heads * HEAD_DIM
    bf16, f32 = jnp.bfloat16, jnp.float32

    bias = pl.pallas_call(
        functools.partial(bias_kernel, grid_rows, grid_cols, tile_rows, tile_cols),
        out_shape=jax.ShapeDtypeStruct((BLOCKS, heads, QUERIES, SLAB), f32),
        in_specs=[VMEM],
        out_specs=VMEM,
        scratch_shapes=[pltpu.VMEM((LAYERS, heads, SPAN, BLOCK_COLS, LANES), f32)],
        compiler_params=pltpu.CompilerParams(vmem_limit_bytes=16 * 2**20),
        cost_estimate=pl.CostEstimate(flops=4 * 10**6, bytes_accessed=6 * 2**20, transcendentals=0),
        name="bias",
    )(bias_rows(offset_bias))

    above, below = shifts(grid_tokens, "sp")
    column = jnp.concatenate((above, grid_tokens, below), axis=0)
    left, right = shifts(column, "tp")

    rows, cols = 3 * tile_rows, 3 * tile_cols
    region_rows, region_cols = 2 * tile_rows, 2 * tile_cols
    return pl.pallas_call(
        layers_kernel,
        out_shape=jax.ShapeDtypeStruct(grid_tokens.shape, grid_tokens.dtype),
        in_specs=[VMEM] * 9,
        out_specs=VMEM,
        scratch_shapes=[
            pltpu.VMEM((rows, cols, width), bf16),
            pltpu.VMEM((rows, region_cols, width), bf16),
            pltpu.VMEM((rows, cols, inner), bf16),
            pltpu.VMEM((rows, cols, inner), bf16),
            pltpu.VMEM((region_rows, region_cols, inner), bf16),
            pltpu.VMEM((region_rows, region_cols, inner), bf16),
            pltpu.VMEM((region_rows, region_cols, width), f32),
            pltpu.VMEM((region_rows, tile_cols, width), f32),
        ],
        compiler_params=pltpu.CompilerParams(vmem_limit_bytes=40 * 2**20),
        cost_estimate=pl.CostEstimate(
            flops=6 * 10**9, bytes_accessed=16 * 2**20, transcendentals=10**6
        ),
        name="layers",
    )(left, column, right, norm_gain, w_query, w_key, w_value, w_out, bias)


def solution(mesh):
    return jax.shard_map(
        on_device,
        mesh=mesh,
        in_specs=(P(("grp", "sp"), "tp", None), P(), P(), P(), P(), P(), P()),
        out_specs=P(("grp", "sp"), "tp", None),
        check_vma=False,
    )
```

```python
import functools
import math

import jax
import jax.numpy as jnp
from jax import lax
from jax.experimental import pallas as pl
from jax.experimental.pallas import tpu as pltpu
from jax.sharding import PartitionSpec as P

HEAD_DIM = 128
WIN_ROWS = 8
WIN_COLS = 16
LAYERS = 2
HALF_ROWS = WIN_ROWS // 2
HALF_COLS = WIN_COLS // 2

NORM_EPSILON = 1e-06
LOG2E = math.log2(math.e)
MASKED = -1e30

BLOCK_ROWS = 8
BLOCK_COLS = 16
SLAB_ROWS = BLOCK_ROWS + WIN_ROWS
SLAB_COLS = BLOCK_COLS + WIN_COLS
QUERIES = BLOCK_ROWS * BLOCK_COLS
SLAB = SLAB_ROWS * SLAB_COLS
LANES = 128
GROUP = LANES // SLAB_COLS
SPAN = SLAB_ROWS - GROUP + BLOCK_ROWS
BLOCKS = 5

TILES = 3
SLOTS = 3
CHUNK = 32

ORDER = ((0, -1), (-1, 0), (-1, -1), (-1, 1), (1, -1), (0, 1), (1, 0), (1, 1))

VMEM = pl.BlockSpec(memory_space=pltpu.VMEM)


def bias_rows(table):
    rows = jnp.transpose(table * LOG2E, (0, 2, 1, 3))
    after = SPAN + GROUP - 1 - HALF_ROWS - rows.shape[1]
    return jnp.pad(rows, ((0, 0), (HALF_ROWS, after), (0, 0), (0, LANES - rows.shape[3])))


def bias_kernel(grid_rows, grid_cols, tile_rows, tile_cols, rows_ref, out_ref, shifted):
    layers, _, heads = rows_ref.shape[:3]
    first_row = lax.axis_index("sp") * tile_rows
    first_col = lax.axis_index("tp") * tile_cols

    for layer in range(layers):
        for u in range(SPAN):
            lines = rows_ref[layer, u]
            for g in range(1, GROUP):
                lines = lines + pltpu.roll(rows_ref[layer, u + g], g * SLAB_COLS, 1)
            for head in range(heads):
                shifted[layer, head, u] = pltpu.roll(
                    jnp.broadcast_to(lines[head : head + 1], (BLOCK_COLS, LANES)),
                    LANES - (HALF_COLS - 1),
                    1,
                    stride=1,
                    stride_axis=0,
                )

    lane = lax.broadcasted_iota(jnp.int32, (BLOCK_COLS, LANES), 1)
    column = lax.broadcasted_iota(jnp.int32, (BLOCK_COLS, LANES), 0)
    key_col = lane % SLAB_COLS
    key_row = lane // SLAB_COLS

    def block(index, _):
        last = index // (BLOCKS - 1)
        row_block, col_block = (index // 2) % 2, index % 2
        row0 = first_row + (1 - last) * (row_block * BLOCK_ROWS - HALF_ROWS)
        col0 = first_col + (1 - last) * (col_block * BLOCK_COLS - HALF_COLS)
        col_start = jnp.clip(col0 + column - HALF_COLS, 0, grid_cols - WIN_COLS)
        behind = col0 - HALF_COLS + key_col - col_start
        col_inside = (behind >= 0) & (behind < WIN_COLS)
        for i in range(BLOCK_ROWS):
            row_start = jnp.clip(row0 + i - HALF_ROWS, 0, grid_rows - WIN_ROWS)
            for j in range(SLAB_ROWS // GROUP):
                below = key_row + (row0 - HALF_ROWS + j * GROUP - row_start)
                inside = col_inside & (below >= 0) & (below < WIN_ROWS)
                for head in range(heads):
                    out_ref[
                        index,
                        head,
                        i * BLOCK_COLS : (i + 1) * BLOCK_COLS,
                        j * LANES : (j + 1) * LANES,
                    ] = jnp.where(
                        inside, shifted[last, head, GROUP * j - i + BLOCK_ROWS - 1], MASKED
                    )
        return 0

    lax.fori_loop(0, BLOCKS, block, 0)


def normed_rows(values, gain):
    factor = lax.rsqrt(jnp.mean(values * values, axis=-1, keepdims=True) + NORM_EPSILON)
    return values * factor * gain


def project(cells, weight):
    rows, cols, width = cells.shape
    out = jnp.dot(
        cells.reshape(rows * cols, width), weight, preferred_element_type=jnp.float32
    )
    return out.astype(jnp.bfloat16).reshape(rows, cols, weight.shape[1])


def layers_kernel(*refs):
    tiles, refs = refs[: TILES * TILES], refs[TILES * TILES :]
    gain, w_query, w_key, w_value, w_out, bias, out_ref = refs[:7]
    normed, normed_q, keys, values, queries, mixture, branch, center, scores, weights = refs[7:]
    f32, bf16 = jnp.float32, jnp.bfloat16
    heads = w_query.shape[2] // HEAD_DIM
    rows, cols = normed.shape[:2]
    region_rows, region_cols = mixture.shape[:2]
    slots = scores.shape[0]

    def put_values(where, out):
        for head in range(heads):
            values[(*where, pl.ds(2 * head * HEAD_DIM, HEAD_DIM))] = out[
                :, :, head * HEAD_DIM : (head + 1) * HEAD_DIM
            ]

    def attend(units):
        def products(step):
            _, head, tile, slab = units[step]
            lanes = pl.ds(head * HEAD_DIM, HEAD_DIM)
            scores[step % slots] = lax.dot_general(
                queries[(*tile, lanes)].reshape(QUERIES, HEAD_DIM),
                keys[(*slab, lanes)].reshape(SLAB, HEAD_DIM),
                (((1,), (1,)), ((), ())),
                preferred_element_type=f32,
            )

        def softmax(step):
            block, head, _, _ = units[step]
            for first in range(0, QUERIES, CHUNK):
                part = pl.ds(first, CHUNK)
                shifted = scores[step % slots, part] * (LOG2E / HEAD_DIM**0.5)
                shifted = shifted + bias[block, head, part]
                top = jnp.max(shifted, axis=1, keepdims=True)
                weights[step % slots, part] = jnp.exp2(shifted - top).astype(bf16)

        def mix(step):
            _, head, tile, slab = units[step]
            both = jnp.dot(
                weights[step % slots],
                values[(*slab, pl.ds(2 * head * HEAD_DIM, 2 * HEAD_DIM))].reshape(
                    SLAB, 2 * HEAD_DIM
                ),
                preferred_element_type=f32,
            )
            out = (both[:, :HEAD_DIM] / both[:, HEAD_DIM:]).astype(bf16)
            mixture[(*tile, pl.ds(head * HEAD_DIM, HEAD_DIM))] = out.reshape(
                BLOCK_ROWS, BLOCK_COLS, HEAD_DIM
            )

        for step in range(len(units) + 2):
            if step < len(units):
                products(step)
            if 0 <= step - 1 < len(units):
                softmax(step - 1)
            if 0 <= step - 2:
                mix(step - 2)

    def part_of(r, c):
        return tiles[r // BLOCK_ROWS * TILES + c][r % BLOCK_ROWS].astype(f32)

    for head in range(heads):
        values[:, :, pl.ds((2 * head + 1) * HEAD_DIM, HEAD_DIM)] = jnp.ones(
            (rows, cols, HEAD_DIM), bf16
        )
    for r in range(rows):
        parts = [normed_rows(part_of(r, c), gain[0:1]) for c in range(TILES)]
        for index, part in enumerate(parts):
            normed[r, index * BLOCK_COLS : (index + 1) * BLOCK_COLS] = part.astype(bf16)
        if 0 <= r - HALF_ROWS < region_rows:
            for index in range(2):
                both = (parts[index][HALF_COLS:], parts[index + 1][:HALF_COLS])
                normed_q[r - HALF_ROWS, index * BLOCK_COLS : (index + 1) * BLOCK_COLS] = (
                    jnp.concatenate(both, axis=0).astype(bf16)
                )
        if r % BLOCK_ROWS == BLOCK_ROWS - 1:
            band = pl.ds(r + 1 - BLOCK_ROWS, BLOCK_ROWS)
            keys[band] = project(normed[band], w_key[0])
            put_values((band, slice(None)), project(normed[band], w_value[0]))
    queries[...] = project(normed_q[...], w_query[0])

    units = []
    for index in range(BLOCKS - 1):
        row, col = index // 2 * BLOCK_ROWS, index % 2 * BLOCK_COLS
        tile = (pl.ds(row, BLOCK_ROWS), pl.ds(col, BLOCK_COLS))
        slab = (pl.ds(row, SLAB_ROWS), pl.ds(col, SLAB_COLS))
        units += [(index, head, tile, slab) for head in range(heads)]
    attend(units)
    branch[...] = jnp.dot(
        mixture[...].reshape(region_rows * region_cols, heads * HEAD_DIM),
        w_out[0],
        preferred_element_type=f32,
    ).reshape(branch.shape)

    own = pl.ds(HALF_ROWS, BLOCK_ROWS)
    inner = slice(HALF_COLS, HALF_COLS + BLOCK_COLS)
    for r in range(region_rows):
        before, here, after = (part_of(r + HALF_ROWS, c) for c in range(TILES))
        tokens = jnp.concatenate((before[HALF_COLS:], here, after[:HALF_COLS]), axis=0)
        stream = (tokens + branch[r]).astype(bf16).astype(f32)
        part = normed_rows(stream, gain[1:2])
        normed[r, :region_cols] = part.astype(bf16)
        if 0 <= r - HALF_ROWS < BLOCK_ROWS:
            normed_q[r - HALF_ROWS, :BLOCK_COLS] = part[inner].astype(bf16)
            center[r - HALF_ROWS] = stream[inner]
    region = (pl.ds(0, region_rows), pl.ds(0, region_cols))
    tile = (pl.ds(0, BLOCK_ROWS), pl.ds(0, BLOCK_COLS))
    keys[region] = project(normed[region], w_key[1])
    put_values(region, project(normed[region], w_value[1]))
    queries[tile] = project(normed_q[tile], w_query[1])
    attend([(BLOCKS - 1, head, tile, region) for head in range(heads)])
    last = jnp.dot(
        mixture[tile].reshape(QUERIES, heads * HEAD_DIM), w_out[1], preferred_element_type=f32
    )
    out_ref[...] = (center[...] + last.reshape(out_ref.shape)).astype(out_ref.dtype)


def from_offset(cells, row, col):
    rows, cols = lax.axis_size("sp"), lax.axis_size("tp")
    pairs = [
        ((r + row) * cols + c + col, r * cols + c)
        for r in range(rows)
        for c in range(cols)
        if 0 <= r + row < rows and 0 <= c + col < cols
    ]
    return lax.ppermute(cells, ("sp", "tp"), pairs)


def on_device(grid_tokens, norm_gain, w_query, w_key, w_value, offset_bias, w_out):
    tile_rows, tile_cols, width = grid_tokens.shape
    grid_rows = tile_rows * lax.axis_size("sp")
    grid_cols = tile_cols * lax.axis_size("tp")
    heads = offset_bias.shape[1]
    inner = heads * HEAD_DIM
    bf16, f32 = jnp.bfloat16, jnp.float32

    bias = pl.pallas_call(
        functools.partial(bias_kernel, grid_rows, grid_cols, tile_rows, tile_cols),
        out_shape=jax.ShapeDtypeStruct((BLOCKS, heads, QUERIES, SLAB), f32),
        in_specs=[VMEM],
        out_specs=VMEM,
        scratch_shapes=[pltpu.VMEM((LAYERS, heads, SPAN, BLOCK_COLS, LANES), f32)],
        compiler_params=pltpu.CompilerParams(vmem_limit_bytes=8 * 2**20),
        cost_estimate=pl.CostEstimate(flops=4 * 10**6, bytes_accessed=6 * 2**20, transcendentals=0),
        name="bias",
    )(bias_rows(offset_bias))

    arrived = {(0, 0): grid_tokens}
    for offset in ORDER:
        arrived[offset] = from_offset(grid_tokens, *offset)
    tiles = [arrived[(row, col)] for row in (-1, 0, 1) for col in (-1, 0, 1)]

    rows, cols = TILES * tile_rows, TILES * tile_cols
    region_rows, region_cols = 2 * tile_rows, 2 * tile_cols
    return pl.pallas_call(
        layers_kernel,
        out_shape=jax.ShapeDtypeStruct(grid_tokens.shape, grid_tokens.dtype),
        in_specs=[VMEM] * (len(tiles) + 6),
        out_specs=VMEM,
        scratch_shapes=[
            pltpu.VMEM((rows, cols, width), bf16),
            pltpu.VMEM((region_rows, region_cols, width), bf16),
            pltpu.VMEM((rows, cols, inner), bf16),
            pltpu.VMEM((rows, cols, 2 * inner), bf16),
            pltpu.VMEM((region_rows, region_cols, inner), bf16),
            pltpu.VMEM((region_rows, region_cols, inner), bf16),
            pltpu.VMEM((region_rows, region_cols, width), f32),
            pltpu.VMEM((tile_rows, tile_cols, width), f32),
            pltpu.VMEM((SLOTS, QUERIES, SLAB), f32),
            pltpu.VMEM((SLOTS, QUERIES, SLAB), bf16),
        ],
        compiler_params=pltpu.CompilerParams(vmem_limit_bytes=24 * 2**20),
        cost_estimate=pl.CostEstimate(
            flops=6 * 10**9, bytes_accessed=16 * 2**20, transcendentals=10**6
        ),
        name="layers",
    )(*tiles, norm_gain, w_query, w_key, w_value, w_out, bias)


def solution(mesh):
    return jax.shard_map(
        on_device,
        mesh=mesh,
        in_specs=(P(("grp", "sp"), "tp", None), P(), P(), P(), P(), P(), P()),
        out_specs=P(("grp", "sp"), "tp", None),
        check_vma=False,
    )
```

```python
import functools
import math

import jax
import jax.numpy as jnp
from jax import lax
from jax.experimental import pallas as pl
from jax.experimental.pallas import tpu as pltpu
from jax.sharding import PartitionSpec as P

HEAD_DIM = 128
WIN_ROWS = 8
WIN_COLS = 16
LAYERS = 2
HALF_ROWS = WIN_ROWS // 2
HALF_COLS = WIN_COLS // 2

NORM_EPSILON = 1e-06
LOG2E = math.log2(math.e)
MASKED = -1e30

BLOCK_ROWS = 8
BLOCK_COLS = 16
SLAB_ROWS = BLOCK_ROWS + WIN_ROWS
SLAB_COLS = BLOCK_COLS + WIN_COLS
QUERIES = BLOCK_ROWS * BLOCK_COLS
SLAB = SLAB_ROWS * SLAB_COLS
LANES = 128
GROUP = LANES // SLAB_COLS
SPAN = SLAB_ROWS - GROUP + BLOCK_ROWS
BLOCKS = 5

TILES = 3
SLOTS = 3
CHUNK = 32

ORDER = ((0, -1), (-1, 0), (-1, -1), (-1, 1), (1, -1), (1, 0), (1, 1), (0, 1))

VMEM = pl.BlockSpec(memory_space=pltpu.VMEM)
HBM = pl.BlockSpec(memory_space=pltpu.HBM)


def bias_kernel(grid_rows, grid_cols, tile_rows, tile_cols, table, out_ref, lines, shifted):
    layers, offsets, heads = table.shape[:3]
    first_row = lax.axis_index("sp") * tile_rows
    first_col = lax.axis_index("tp") * tile_cols

    blank = jnp.zeros((heads, LANES - table.shape[3]), jnp.float32)
    for layer in range(layers):
        rows = [
            jnp.concatenate((table[layer, o] * LOG2E, blank), axis=1) for o in range(offsets)
        ]
        turned = [[pltpu.roll(row, g * SLAB_COLS, 1) if g else row for row in rows] for g in range(GROUP)]
        for u in range(SPAN):
            line = jnp.zeros((heads, LANES), jnp.float32)
            for g in range(GROUP):
                if 0 <= u + g - HALF_ROWS < offsets:
                    line = line + turned[g][u + g - HALF_ROWS]
            lines[layer, u] = line
        for head in range(heads):
            for u in range(SPAN):
                shifted[layer, head, u] = pltpu.roll(
                    jnp.broadcast_to(lines[layer, u, head : head + 1], (BLOCK_COLS, LANES)),
                    LANES - (HALF_COLS - 1),
                    1,
                    stride=1,
                    stride_axis=0,
                )

    lane = lax.broadcasted_iota(jnp.int32, (BLOCK_COLS, LANES), 1)
    column = lax.broadcasted_iota(jnp.int32, (BLOCK_COLS, LANES), 0)
    key_col = lane % SLAB_COLS
    key_row = lane // SLAB_COLS

    def block(index, _):
        last = index // (BLOCKS - 1)
        row_block, col_block = (index // 2) % 2, index % 2
        row0 = first_row + (1 - last) * (row_block * BLOCK_ROWS - HALF_ROWS)
        col0 = first_col + (1 - last) * (col_block * BLOCK_COLS - HALF_COLS)
        col_start = jnp.clip(col0 + column - HALF_COLS, 0, grid_cols - WIN_COLS)
        behind = col0 - HALF_COLS + key_col - col_start
        col_inside = (behind >= 0) & (behind < WIN_COLS)
        for i in range(BLOCK_ROWS):
            row_start = jnp.clip(row0 + i - HALF_ROWS, 0, grid_rows - WIN_ROWS)
            for j in range(SLAB_ROWS // GROUP):
                below = key_row + (row0 - HALF_ROWS + j * GROUP - row_start)
                inside = col_inside & (below >= 0) & (below < WIN_ROWS)
                for head in range(heads):
                    out_ref[
                        index,
                        head,
                        i * BLOCK_COLS : (i + 1) * BLOCK_COLS,
                        j * LANES : (j + 1) * LANES,
                    ] = jnp.where(
                        inside, shifted[last, head, GROUP * j - i + BLOCK_ROWS - 1], MASKED
                    )
        return 0

    lax.fori_loop(0, BLOCKS, block, 0)


def normed_rows(values, gain):
    factor = lax.rsqrt(jnp.mean(values * values, axis=-1, keepdims=True) + NORM_EPSILON)
    return values * factor * gain


def project(cells, weight):
    rows, cols, width = cells.shape
    out = jnp.dot(
        cells.reshape(rows * cols, width), weight, preferred_element_type=jnp.float32
    )
    return out.astype(jnp.bfloat16).reshape(rows, cols, weight.shape[1])


def layers_kernel(*refs):
    tiles, refs = refs[: TILES * TILES], refs[TILES * TILES :]
    gain, query_source, w_key, w_value, out_source, bias, out_ref = refs[:7]
    normed, normed_q, keys, values, queries, mixture, branch, center, scores, weights = refs[7:17]
    w_query, w_out, arrivals = refs[17:]
    loads = [
        pltpu.make_async_copy(query_source, w_query, arrivals.at[0]),
        pltpu.make_async_copy(out_source, w_out, arrivals.at[1]),
    ]
    for load in loads:
        load.start()
    f32, bf16 = jnp.float32, jnp.bfloat16
    heads = w_query.shape[2] // HEAD_DIM
    rows, cols = normed.shape[:2]
    region_rows, region_cols = mixture.shape[:2]
    slots = scores.shape[0]

    def put_values(where, out):
        for head in range(heads):
            values[(*where, pl.ds(2 * head * HEAD_DIM, HEAD_DIM))] = out[
                :, :, head * HEAD_DIM : (head + 1) * HEAD_DIM
            ]

    def attend(units):
        def products(step):
            _, head, tile, slab = units[step]
            lanes = pl.ds(head * HEAD_DIM, HEAD_DIM)
            scores[step % slots] = lax.dot_general(
                queries[(*tile, lanes)].reshape(QUERIES, HEAD_DIM),
                keys[(*slab, lanes)].reshape(SLAB, HEAD_DIM),
                (((1,), (1,)), ((), ())),
                preferred_element_type=f32,
            )

        def softmax(step):
            block, head, _, _ = units[step]
            for first in range(0, QUERIES, CHUNK):
                part = pl.ds(first, CHUNK)
                shifted = scores[step % slots, part] * (LOG2E / HEAD_DIM**0.5)
                shifted = shifted + bias[block, head, part]
                top = jnp.max(shifted, axis=1, keepdims=True)
                weights[step % slots, part] = jnp.exp2(shifted - top).astype(bf16)

        def mix(step):
            _, head, tile, slab = units[step]
            both = jnp.dot(
                weights[step % slots],
                values[(*slab, pl.ds(2 * head * HEAD_DIM, 2 * HEAD_DIM))].reshape(
                    SLAB, 2 * HEAD_DIM
                ),
                preferred_element_type=f32,
            )
            out = (both[:, :HEAD_DIM] / both[:, HEAD_DIM:]).astype(bf16)
            mixture[(*tile, pl.ds(head * HEAD_DIM, HEAD_DIM))] = out.reshape(
                BLOCK_ROWS, BLOCK_COLS, HEAD_DIM
            )

        for step in range(len(units) + 2):
            if step < len(units):
                products(step)
            if 0 <= step - 1 < len(units):
                softmax(step - 1)
            if 0 <= step - 2:
                mix(step - 2)

    def part_of(r, c):
        return tiles[r // BLOCK_ROWS * TILES + c][r % BLOCK_ROWS].astype(f32)

    for head in range(heads):
        values[:, :, pl.ds((2 * head + 1) * HEAD_DIM, HEAD_DIM)] = jnp.ones(
            (rows, cols, HEAD_DIM), bf16
        )
    for r in range(rows):
        parts = [normed_rows(part_of(r, c), gain[0:1]) for c in range(TILES)]
        for index, part in enumerate(parts):
            normed[r, index * BLOCK_COLS : (index + 1) * BLOCK_COLS] = part.astype(bf16)
        if 0 <= r - HALF_ROWS < region_rows:
            for index in range(2):
                both = (parts[index][HALF_COLS:], parts[index + 1][:HALF_COLS])
                normed_q[r - HALF_ROWS, index * BLOCK_COLS : (index + 1) * BLOCK_COLS] = (
                    jnp.concatenate(both, axis=0).astype(bf16)
                )
        if r % BLOCK_ROWS == BLOCK_ROWS - 1:
            band = pl.ds(r + 1 - BLOCK_ROWS, BLOCK_ROWS)
            keys[band] = project(normed[band], w_key[0])
            put_values((band, slice(None)), project(normed[band], w_value[0]))
    for load in loads:
        load.wait()
    queries[...] = project(normed_q[...], w_query[0])

    units = []
    for index in range(BLOCKS - 1):
        row, col = index // 2 * BLOCK_ROWS, index % 2 * BLOCK_COLS
        tile = (pl.ds(row, BLOCK_ROWS), pl.ds(col, BLOCK_COLS))
        slab = (pl.ds(row, SLAB_ROWS), pl.ds(col, SLAB_COLS))
        units += [(index, head, tile, slab) for head in range(heads)]
    attend(units)
    branch[...] = jnp.dot(
        mixture[...].reshape(region_rows * region_cols, heads * HEAD_DIM),
        w_out[0],
        preferred_element_type=f32,
    ).reshape(branch.shape)

    own = pl.ds(HALF_ROWS, BLOCK_ROWS)
    inner = slice(HALF_COLS, HALF_COLS + BLOCK_COLS)
    for r in range(region_rows):
        before, here, after = (part_of(r + HALF_ROWS, c) for c in range(TILES))
        tokens = jnp.concatenate((before[HALF_COLS:], here, after[:HALF_COLS]), axis=0)
        stream = (tokens + branch[r]).astype(bf16).astype(f32)
        part = normed_rows(stream, gain[1:2])
        normed[r, :region_cols] = part.astype(bf16)
        if 0 <= r - HALF_ROWS < BLOCK_ROWS:
            normed_q[r - HALF_ROWS, :BLOCK_COLS] = part[inner].astype(bf16)
            center[r - HALF_ROWS] = stream[inner]
    region = (pl.ds(0, region_rows), pl.ds(0, region_cols))
    tile = (pl.ds(0, BLOCK_ROWS), pl.ds(0, BLOCK_COLS))
    keys[region] = project(normed[region], w_key[1])
    put_values(region, project(normed[region], w_value[1]))
    queries[tile] = project(normed_q[tile], w_query[1])
    attend([(BLOCKS - 1, head, tile, region) for head in range(heads)])
    last = jnp.dot(
        mixture[tile].reshape(QUERIES, heads * HEAD_DIM), w_out[1], preferred_element_type=f32
    )
    out_ref[...] = (center[...] + last.reshape(out_ref.shape)).astype(out_ref.dtype)


def from_offset(cells, row, col):
    rows, cols = lax.axis_size("sp"), lax.axis_size("tp")
    pairs = [
        ((r + row) * cols + c + col, r * cols + c)
        for r in range(rows)
        for c in range(cols)
        if 0 <= r + row < rows and 0 <= c + col < cols
    ]
    return lax.ppermute(cells, ("sp", "tp"), pairs)


def on_device(grid_tokens, norm_gain, w_query, w_key, w_value, offset_bias, w_out):
    tile_rows, tile_cols, width = grid_tokens.shape
    grid_rows = tile_rows * lax.axis_size("sp")
    grid_cols = tile_cols * lax.axis_size("tp")
    heads = offset_bias.shape[1]
    inner = heads * HEAD_DIM
    bf16, f32 = jnp.bfloat16, jnp.float32

    bias = pl.pallas_call(
        functools.partial(bias_kernel, grid_rows, grid_cols, tile_rows, tile_cols),
        out_shape=jax.ShapeDtypeStruct((BLOCKS, heads, QUERIES, SLAB), f32),
        in_specs=[VMEM],
        out_specs=VMEM,
        scratch_shapes=[
            pltpu.VMEM((LAYERS, SPAN, heads, LANES), f32),
            pltpu.VMEM((LAYERS, heads, SPAN, BLOCK_COLS, LANES), f32),
        ],
        compiler_params=pltpu.CompilerParams(vmem_limit_bytes=8 * 2**20),
        cost_estimate=pl.CostEstimate(flops=4 * 10**6, bytes_accessed=32 * 2**20, transcendentals=0),
        name="bias",
    )(jnp.transpose(offset_bias, (0, 2, 1, 3)))

    arrived = {(0, 0): grid_tokens}
    for offset in ORDER:
        arrived[offset] = from_offset(grid_tokens, *offset)
    tiles = [arrived[(row, col)] for row in (-1, 0, 1) for col in (-1, 0, 1)]

    rows, cols = TILES * tile_rows, TILES * tile_cols
    region_rows, region_cols = 2 * tile_rows, 2 * tile_cols
    return pl.pallas_call(
        layers_kernel,
        out_shape=jax.ShapeDtypeStruct(grid_tokens.shape, grid_tokens.dtype),
        in_specs=[VMEM] * (len(tiles) + 1) + [HBM, VMEM, VMEM, HBM, VMEM],
        out_specs=VMEM,
        scratch_shapes=[
            pltpu.VMEM((rows, cols, width), bf16),
            pltpu.VMEM((region_rows, region_cols, width), bf16),
            pltpu.VMEM((rows, cols, inner), bf16),
            pltpu.VMEM((rows, cols, 2 * inner), bf16),
            pltpu.VMEM((region_rows, region_cols, inner), bf16),
            pltpu.VMEM((region_rows, region_cols, inner), bf16),
            pltpu.VMEM((region_rows, region_cols, width), f32),
            pltpu.VMEM((tile_rows, tile_cols, width), f32),
            pltpu.VMEM((SLOTS, QUERIES, SLAB), f32),
            pltpu.VMEM((SLOTS, QUERIES, SLAB), bf16),
            pltpu.VMEM(w_query.shape, bf16),
            pltpu.VMEM(w_out.shape, bf16),
            pltpu.SemaphoreType.DMA((2,)),
        ],
        compiler_params=pltpu.CompilerParams(vmem_limit_bytes=24 * 2**20),
        cost_estimate=pl.CostEstimate(
            flops=6 * 10**9, bytes_accessed=16 * 2**20, transcendentals=10**6
        ),
        name="layers",
    )(
        *tiles,
        norm_gain,
        pltpu.with_memory_space_constraint(w_query, pltpu.HBM),
        w_key,
        w_value,
        pltpu.with_memory_space_constraint(w_out, pltpu.HBM),
        bias,
    )


def solution(mesh):
    return jax.shard_map(
        on_device,
        mesh=mesh,
        in_specs=(P(("grp", "sp"), "tp", None), P(), P(), P(), P(), P(), P()),
        out_specs=P(("grp", "sp"), "tp", None),
        check_vma=False,
    )
```

```python
import functools
import math

import jax
import jax.numpy as jnp
from jax import lax
from jax.experimental import pallas as pl
from jax.experimental.pallas import tpu as pltpu
from jax.sharding import PartitionSpec as P

HEAD_DIM = 128
WIN_ROWS = 8
WIN_COLS = 16
LAYERS = 2
HALF_ROWS = WIN_ROWS // 2
HALF_COLS = WIN_COLS // 2

NORM_EPSILON = 1e-06
LOG2E = math.log2(math.e)
MASKED = -1e30

BLOCK_ROWS = 8
BLOCK_COLS = 16
SLAB_ROWS = BLOCK_ROWS + WIN_ROWS
SLAB_COLS = BLOCK_COLS + WIN_COLS
QUERIES = BLOCK_ROWS * BLOCK_COLS
SLAB = SLAB_ROWS * SLAB_COLS
LANES = 128
GROUP = LANES // SLAB_COLS
SPAN = SLAB_ROWS - GROUP + BLOCK_ROWS
BLOCKS = 5

TILES = 3
SLOTS = 3
CHUNK = 32

ORDER = ((0, -1), (-1, 0), (-1, -1), (-1, 1), (1, -1), (1, 0), (1, 1), (0, 1))

VMEM = pl.BlockSpec(memory_space=pltpu.VMEM)
HBM = pl.BlockSpec(memory_space=pltpu.HBM)


def fill_bias(grid, table_source, table, lines, shifted, out_ref, arrival):
    grid_rows, grid_cols, tile_rows, tile_cols = grid
    layers, offsets, heads = table.shape[:3]
    first_row = lax.axis_index("sp") * tile_rows
    first_col = lax.axis_index("tp") * tile_cols
    load = pltpu.make_async_copy(table_source, table, arrival)
    load.start()
    load.wait()

    blank = jnp.zeros((heads, LANES - table.shape[3]), jnp.float32)
    for layer in range(layers):
        rows = [
            jnp.concatenate((table[layer, o] * LOG2E, blank), axis=1) for o in range(offsets)
        ]
        turned = [[pltpu.roll(row, g * SLAB_COLS, 1) if g else row for row in rows] for g in range(GROUP)]
        for u in range(SPAN):
            line = jnp.zeros((heads, LANES), jnp.float32)
            for g in range(GROUP):
                if 0 <= u + g - HALF_ROWS < offsets:
                    line = line + turned[g][u + g - HALF_ROWS]
            lines[layer, u] = line
        for head in range(heads):
            for u in range(SPAN):
                shifted[layer, head, u] = pltpu.roll(
                    jnp.broadcast_to(lines[layer, u, head : head + 1], (BLOCK_COLS, LANES)),
                    LANES - (HALF_COLS - 1),
                    1,
                    stride=1,
                    stride_axis=0,
                )

    lane = lax.broadcasted_iota(jnp.int32, (BLOCK_COLS, LANES), 1)
    column = lax.broadcasted_iota(jnp.int32, (BLOCK_COLS, LANES), 0)
    key_col = lane % SLAB_COLS
    key_row = lane // SLAB_COLS

    def block(index, _):
        last = index // (BLOCKS - 1)
        row_block, col_block = (index // 2) % 2, index % 2
        row0 = first_row + (1 - last) * (row_block * BLOCK_ROWS - HALF_ROWS)
        col0 = first_col + (1 - last) * (col_block * BLOCK_COLS - HALF_COLS)
        col_start = jnp.clip(col0 + column - HALF_COLS, 0, grid_cols - WIN_COLS)
        behind = col0 - HALF_COLS + key_col - col_start
        col_inside = (behind >= 0) & (behind < WIN_COLS)
        for i in range(BLOCK_ROWS):
            row_start = jnp.clip(row0 + i - HALF_ROWS, 0, grid_rows - WIN_ROWS)
            for j in range(SLAB_ROWS // GROUP):
                below = key_row + (row0 - HALF_ROWS + j * GROUP - row_start)
                inside = col_inside & (below >= 0) & (below < WIN_ROWS)
                for head in range(heads):
                    out_ref[
                        index,
                        head,
                        i * BLOCK_COLS : (i + 1) * BLOCK_COLS,
                        j * LANES : (j + 1) * LANES,
                    ] = jnp.where(
                        inside, shifted[last, head, GROUP * j - i + BLOCK_ROWS - 1], MASKED
                    )
        return 0

    lax.fori_loop(0, BLOCKS, block, 0)


def at_corner():
    return (lax.axis_index("sp") == 0) & (lax.axis_index("tp") == 0)


def bias_kernel(grid, table_source, out_ref, filled, table, lines, shifted, arrival):
    @pl.when(jnp.logical_not(at_corner()))
    def _():
        fill_bias(grid, table_source, table, lines, shifted, filled, arrival.at[0])
        store = pltpu.make_async_copy(filled, out_ref, arrival.at[0])
        store.start()
        store.wait()


def normed_rows(values, gain):
    factor = lax.rsqrt(jnp.mean(values * values, axis=-1, keepdims=True) + NORM_EPSILON)
    return values * factor * gain


def project(cells, weight):
    rows, cols, width = cells.shape
    out = jnp.dot(
        cells.reshape(rows * cols, width), weight, preferred_element_type=jnp.float32
    )
    return out.astype(jnp.bfloat16).reshape(rows, cols, weight.shape[1])


def layers_kernel(grid, *refs):
    tiles, refs = refs[: TILES * TILES], refs[TILES * TILES :]
    gain, query_source, w_key, w_value, out_source, table_source, bias_source, out_ref = refs[:8]
    normed, normed_q, keys, values, queries, mixture, branch, center, scores, weights = refs[8:18]
    w_query, w_out, bias, table, lines, shifted, arrivals = refs[18:]
    loads = [
        pltpu.make_async_copy(bias_source, bias, arrivals.at[2]),
        pltpu.make_async_copy(query_source, w_query, arrivals.at[0]),
        pltpu.make_async_copy(out_source, w_out, arrivals.at[1]),
    ]
    for load in loads:
        load.start()
    f32, bf16 = jnp.float32, jnp.bfloat16
    heads = w_query.shape[2] // HEAD_DIM
    rows, cols = normed.shape[:2]
    region_rows, region_cols = mixture.shape[:2]
    slots = scores.shape[0]

    def put_values(where, out):
        for head in range(heads):
            values[(*where, pl.ds(2 * head * HEAD_DIM, HEAD_DIM))] = out[
                :, :, head * HEAD_DIM : (head + 1) * HEAD_DIM
            ]

    def attend(units):
        def products(step):
            _, head, tile, slab = units[step]
            lanes = pl.ds(head * HEAD_DIM, HEAD_DIM)
            scores[step % slots] = lax.dot_general(
                queries[(*tile, lanes)].reshape(QUERIES, HEAD_DIM),
                keys[(*slab, lanes)].reshape(SLAB, HEAD_DIM),
                (((1,), (1,)), ((), ())),
                preferred_element_type=f32,
            )

        def softmax(step):
            block, head, _, _ = units[step]
            for first in range(0, QUERIES, CHUNK):
                part = pl.ds(first, CHUNK)
                shifted = scores[step % slots, part] * (LOG2E / HEAD_DIM**0.5)
                shifted = shifted + bias[block, head, part]
                top = jnp.max(shifted, axis=1, keepdims=True)
                weights[step % slots, part] = jnp.exp2(shifted - top).astype(bf16)

        def mix(step):
            _, head, tile, slab = units[step]
            both = jnp.dot(
                weights[step % slots],
                values[(*slab, pl.ds(2 * head * HEAD_DIM, 2 * HEAD_DIM))].reshape(
                    SLAB, 2 * HEAD_DIM
                ),
                preferred_element_type=f32,
            )
            out = (both[:, :HEAD_DIM] / both[:, HEAD_DIM:]).astype(bf16)
            mixture[(*tile, pl.ds(head * HEAD_DIM, HEAD_DIM))] = out.reshape(
                BLOCK_ROWS, BLOCK_COLS, HEAD_DIM
            )

        for step in range(len(units) + 2):
            if step < len(units):
                products(step)
            if 0 <= step - 1 < len(units):
                softmax(step - 1)
            if 0 <= step - 2:
                mix(step - 2)

    def part_of(r, c):
        return tiles[r // BLOCK_ROWS * TILES + c][r % BLOCK_ROWS].astype(f32)

    for head in range(heads):
        values[:, :, pl.ds((2 * head + 1) * HEAD_DIM, HEAD_DIM)] = jnp.ones(
            (rows, cols, HEAD_DIM), bf16
        )
    for r in range(rows):
        parts = [normed_rows(part_of(r, c), gain[0:1]) for c in range(TILES)]
        for index, part in enumerate(parts):
            normed[r, index * BLOCK_COLS : (index + 1) * BLOCK_COLS] = part.astype(bf16)
        if 0 <= r - HALF_ROWS < region_rows:
            for index in range(2):
                both = (parts[index][HALF_COLS:], parts[index + 1][:HALF_COLS])
                normed_q[r - HALF_ROWS, index * BLOCK_COLS : (index + 1) * BLOCK_COLS] = (
                    jnp.concatenate(both, axis=0).astype(bf16)
                )
        if r % BLOCK_ROWS == BLOCK_ROWS - 1:
            band = pl.ds(r + 1 - BLOCK_ROWS, BLOCK_ROWS)
            keys[band] = project(normed[band], w_key[0])
            put_values((band, slice(None)), project(normed[band], w_value[0]))
    for load in loads:
        load.wait()

    @pl.when(at_corner())
    def _():
        fill_bias(grid, table_source, table, lines, shifted, bias, arrivals.at[0])

    queries[...] = project(normed_q[...], w_query[0])

    units = []
    for index in range(BLOCKS - 1):
        row, col = index // 2 * BLOCK_ROWS, index % 2 * BLOCK_COLS
        tile = (pl.ds(row, BLOCK_ROWS), pl.ds(col, BLOCK_COLS))
        slab = (pl.ds(row, SLAB_ROWS), pl.ds(col, SLAB_COLS))
        units += [(index, head, tile, slab) for head in range(heads)]
    attend(units)
    branch[...] = jnp.dot(
        mixture[...].reshape(region_rows * region_cols, heads * HEAD_DIM),
        w_out[0],
        preferred_element_type=f32,
    ).reshape(branch.shape)

    own = pl.ds(HALF_ROWS, BLOCK_ROWS)
    inner = slice(HALF_COLS, HALF_COLS + BLOCK_COLS)
    for r in range(region_rows):
        before, here, after = (part_of(r + HALF_ROWS, c) for c in range(TILES))
        tokens = jnp.concatenate((before[HALF_COLS:], here, after[:HALF_COLS]), axis=0)
        stream = (tokens + branch[r]).astype(bf16).astype(f32)
        part = normed_rows(stream, gain[1:2])
        normed[r, :region_cols] = part.astype(bf16)
        if 0 <= r - HALF_ROWS < BLOCK_ROWS:
            normed_q[r - HALF_ROWS, :BLOCK_COLS] = part[inner].astype(bf16)
            center[r - HALF_ROWS] = stream[inner]
    region = (pl.ds(0, region_rows), pl.ds(0, region_cols))
    tile = (pl.ds(0, BLOCK_ROWS), pl.ds(0, BLOCK_COLS))
    keys[region] = project(normed[region], w_key[1])
    put_values(region, project(normed[region], w_value[1]))
    queries[tile] = project(normed_q[tile], w_query[1])
    attend([(BLOCKS - 1, head, tile, region) for head in range(heads)])
    last = jnp.dot(
        mixture[tile].reshape(QUERIES, heads * HEAD_DIM), w_out[1], preferred_element_type=f32
    )
    out_ref[...] = (center[...] + last.reshape(out_ref.shape)).astype(out_ref.dtype)


def from_offset(cells, row, col):
    rows, cols = lax.axis_size("sp"), lax.axis_size("tp")
    pairs = [
        ((r + row) * cols + c + col, r * cols + c)
        for r in range(rows)
        for c in range(cols)
        if 0 <= r + row < rows and 0 <= c + col < cols
    ]
    return lax.ppermute(cells, ("sp", "tp"), pairs)


def on_device(grid_tokens, norm_gain, w_query, w_key, w_value, offset_bias, w_out):
    tile_rows, tile_cols, width = grid_tokens.shape
    grid_rows = tile_rows * lax.axis_size("sp")
    grid_cols = tile_cols * lax.axis_size("tp")
    heads = offset_bias.shape[1]
    inner = heads * HEAD_DIM
    bf16, f32 = jnp.bfloat16, jnp.float32

    grid = (grid_rows, grid_cols, tile_rows, tile_cols)
    table = pltpu.with_memory_space_constraint(
        jnp.transpose(offset_bias, (0, 2, 1, 3)), pltpu.HBM
    )
    bias_shape = (BLOCKS, heads, QUERIES, SLAB)
    bias_scratch = [
        pltpu.VMEM(bias_shape, f32),
        pltpu.VMEM(table.shape, f32),
        pltpu.VMEM((LAYERS, SPAN, heads, LANES), f32),
        pltpu.VMEM((LAYERS, heads, SPAN, BLOCK_COLS, LANES), f32),
    ]
    bias = pl.pallas_call(
        functools.partial(bias_kernel, grid),
        out_shape=pltpu.HBM(bias_shape, f32),
        in_specs=[HBM],
        out_specs=HBM,
        scratch_shapes=[*bias_scratch, pltpu.SemaphoreType.DMA((1,))],
        compiler_params=pltpu.CompilerParams(vmem_limit_bytes=16 * 2**20),
        cost_estimate=pl.CostEstimate(
            flops=4 * 10**6, bytes_accessed=32 * 2**20, transcendentals=0
        ),
        name="bias",
    )(table)

    arrived = {(0, 0): grid_tokens}
    for offset in ORDER:
        arrived[offset] = from_offset(grid_tokens, *offset)
    tiles = [arrived[(row, col)] for row in (-1, 0, 1) for col in (-1, 0, 1)]

    rows, cols = TILES * tile_rows, TILES * tile_cols
    region_rows, region_cols = 2 * tile_rows, 2 * tile_cols
    return pl.pallas_call(
        functools.partial(layers_kernel, grid),
        out_shape=jax.ShapeDtypeStruct(grid_tokens.shape, grid_tokens.dtype),
        in_specs=[VMEM] * (len(tiles) + 1) + [HBM, VMEM, VMEM, HBM, HBM, HBM],
        out_specs=VMEM,
        scratch_shapes=[
            pltpu.VMEM((rows, cols, width), bf16),
            pltpu.VMEM((region_rows, region_cols, width), bf16),
            pltpu.VMEM((rows, cols, inner), bf16),
            pltpu.VMEM((rows, cols, 2 * inner), bf16),
            pltpu.VMEM((region_rows, region_cols, inner), bf16),
            pltpu.VMEM((region_rows, region_cols, inner), bf16),
            pltpu.VMEM((region_rows, region_cols, width), f32),
            pltpu.VMEM((tile_rows, tile_cols, width), f32),
            pltpu.VMEM((SLOTS, QUERIES, SLAB), f32),
            pltpu.VMEM((SLOTS, QUERIES, SLAB), bf16),
            pltpu.VMEM(w_query.shape, bf16),
            pltpu.VMEM(w_out.shape, bf16),
            *bias_scratch,
            pltpu.SemaphoreType.DMA((3,)),
        ],
        compiler_params=pltpu.CompilerParams(vmem_limit_bytes=32 * 2**20),
        cost_estimate=pl.CostEstimate(
            flops=6 * 10**9, bytes_accessed=16 * 2**20, transcendentals=10**6
        ),
        name="layers",
    )(
        *tiles,
        norm_gain,
        pltpu.with_memory_space_constraint(w_query, pltpu.HBM),
        w_key,
        w_value,
        pltpu.with_memory_space_constraint(w_out, pltpu.HBM),
        table,
        pltpu.with_memory_space_constraint(bias, pltpu.HBM),
    )


def solution(mesh):
    return jax.shard_map(
        on_device,
        mesh=mesh,
        in_specs=(P(("grp", "sp"), "tp", None), P(), P(), P(), P(), P(), P()),
        out_specs=P(("grp", "sp"), "tp", None),
        check_vma=False,
    )
```
